128 devices in a mesh: rep: 16 (over z, x), fs: 4 (over y), tp: 2 (over core).
Axes of the slice: x: 4, y: 4, z: 4, core: 2. Of those that a mesh axis runs over, the one named last changes fastest.
Arguments:
- inputs: bfloat16 [64, 768, 2048], P(('rep', 'fs'), 'tp'), may hold values from -6 to 6
- pre_gate: bfloat16 [64, 768, 2816], P(('rep', 'fs'), None, 'tp'), may hold values from -6 to 6
- pre_up: bfloat16 [64, 768, 2816], P(('rep', 'fs'), None, 'tp'), may hold values from -6 to 6
- cotangent: bfloat16 [64, 768, 2816], P(('rep', 'fs'), None, 'tp'), may hold values from -16 to 16
- w_gate: bfloat16 [2048, 2816], P('fs', 'tp'), may hold values from -0.125 to 0.125
- w_up: bfloat16 [2048, 2816], P('fs', 'tp'), may hold values from -0.125 to 0.125
- taps_gate: bfloat16 [3, 2816], replicated, may hold values from -3 to 3
- taps_up: bfloat16 [3, 2816], replicated, may hold values from -3 to 3
Outputs:
- grad_inputs: bfloat16 [64, 768, 2048], P(('rep', 'fs'), 'tp')
- grad_w_gate: float32 [2048, 2816], P('fs', 'tp')
- grad_w_up: float32 [2048, 2816], P('fs', 'tp')
- grad_taps_gate: float32 [3, 2816], replicated
- grad_taps_up: float32 [3, 2816], replicated
The draws below stay inside these ranges and needn't reach their ends.
All inputs are finite; a program needn't handle non-finite values.
Results may differ from the reference program's by a relative error of at most 0.0059.
Values may be sent and summed in bfloat16 or wider, within the bound.
No kernel may reach another device: no remote copies, remote signals or barrier semaphores. Data moves between devices by JAX's collectives and lax.ppermute only.
A program may use at most 192 MiB of HBM per device.

```python
import jax
import jax.numpy as jnp
from jax import lax

D = 2048
F = 2816
TAPS = 3
LEN = 768
SEQS = 64
TOKENS = 49152
N_TP = 2


def raised(entries, own_key, source, target, parts, factor):
    def block_of(axis_at):
        return (jnp.arange(entries.shape[axis_at]) // (entries.shape[axis_at] // parts)).reshape((-1,) + (1,) * (entries.ndim - 1 - axis_at))

    first = jax.random.permutation(own_key, parts)[block_of(target)]
    other_side = (block_of(target) + parts // 2) % parts
    return jnp.where((block_of(source) == first) | (block_of(source) == other_side), factor * entries, entries)


def levels(own_key, shape, cuts, low, top_value):
    def one(axis_at, shards_of):
        heights = jax.random.uniform(jax.random.fold_in(jax.random.fold_in(own_key, 6), axis_at), (shards_of,), jnp.float32, low / len(cuts), top_value / len(cuts))
        return jnp.repeat(jnp.exp(heights), shape[axis_at] // shards_of).reshape((-1,) + (1,) * (len(shape) - axis_at - 1))

    gain = one(*cuts[0])
    for cut in cuts[1:]:
        gain = gain * one(*cut)
    return gain


def gaussian(own_key, dims, spread, most, split=(), kind=jnp.bfloat16):
    result = spread * jax.random.normal(own_key, dims, jnp.float32)
    if split:
        result = result * levels(own_key, dims, split, -0.22, 0.18)
    return jnp.clip(result, -most, most).astype(kind)


def noise_with(own_key, shape, spread, limit, split, heavy, held_as=jnp.bfloat16):
    entries = spread * jax.random.normal(own_key, shape, jnp.float32)
    if split:
        entries = entries * levels(own_key, shape, split, -0.22, 0.18)
    return jnp.clip(raised(entries, jax.random.fold_in(own_key, 3), *heavy), -limit, limit).astype(held_as)


def setup_inputs(seed: int = 0) -> dict:
    streams_of = jax.random.split(jax.random.key(seed), 9)
    inputs = gaussian(streams_of[0], (SEQS, LEN, D), 1.0, 6.0, ((0, 64), (1, 2)))
    pre_gate = gaussian(streams_of[1], (SEQS, LEN, F), 1.0, 6.0, ((0, 64), (2, 2)))
    pre_up = gaussian(streams_of[2], (SEQS, LEN, F), 1.0, 6.0, ((0, 64), (2, 2)))
    cotangent = noise_with(streams_of[3], (SEQS, LEN, F), 1.0, 16.0, ((0, 64), (2, 2)), (0, 2, 64, 4.0))
    w_gate = gaussian(streams_of[4], (D, F), D ** -0.5, 0.125, ((0, 4), (1, 2)))
    w_up = gaussian(streams_of[5], (D, F), D ** -0.5, 0.125, ((0, 4), (1, 2)))
    taps_gate = gaussian(streams_of[6], (TAPS, F), 0.6, 3.0)
    taps_up = gaussian(streams_of[7], (TAPS, F), 0.6, 3.0)
    return dict(inputs=inputs, pre_gate=pre_gate, pre_up=pre_up, cotangent=cotangent, w_gate=w_gate, w_up=w_up, taps_gate=taps_gate, taps_up=taps_up)


def causal_mix(signal, kernel):
    length = signal.shape[0]
    padded = jnp.pad(signal, ((2, 0), (0, 0)))
    return kernel[0] * padded[0:length] + kernel[1] * padded[1:length + 1] + kernel[2] * padded[2:length + 2]

def gated_hidden(gate_pre, up_pre, kernel_gate, kernel_up):
    return jax.nn.gelu(causal_mix(gate_pre, kernel_gate)) * causal_mix(up_pre, kernel_up)

def reference(inputs, pre_gate, pre_up, cotangent, w_gate, w_up, taps_gate, taps_up):
    kernel_gate = taps_gate.astype(jnp.float32)
    kernel_up = taps_up.astype(jnp.float32)
    block = F // N_TP

    def one_sequence(totals, item):
        rows, gate_seq, up_seq, back_seq = item
        _, pullback = jax.vjp(gated_hidden, gate_seq.astype(jnp.float32), up_seq.astype(jnp.float32), kernel_gate, kernel_up)
        back_gate, back_up, tap_gate, tap_up = pullback(back_seq.astype(jnp.float32))
        grad_gate = back_gate.astype(jnp.bfloat16)
        grad_up = back_up.astype(jnp.bfloat16)
        summed = jnp.zeros((rows.shape[0], rows.shape[1]), jnp.float32)
        for index in range(N_TP):
            lower = index * block
            partial_value = jnp.dot(grad_gate[:, lower:lower + block], w_gate[:, lower:lower + block].T, preferred_element_type=jnp.float32)
            partial_value = partial_value + jnp.dot(grad_up[:, lower:lower + block], w_up[:, lower:lower + block].T, preferred_element_type=jnp.float32)
            rounded = lax.optimization_barrier(partial_value.astype(jnp.bfloat16))
            summed = summed + rounded.astype(jnp.float32)
        new_totals = (totals[0] + jnp.dot(rows.T, grad_gate, preferred_element_type=jnp.float32), totals[1] + jnp.dot(rows.T, grad_up, preferred_element_type=jnp.float32), totals[2] + tap_gate, totals[3] + tap_up)
        return (new_totals, summed.astype(jnp.bfloat16))
    start = (jnp.zeros((D, F), jnp.float32), jnp.zeros((D, F), jnp.float32), jnp.zeros((TAPS, F), jnp.float32), jnp.zeros((TAPS, F), jnp.float32))
    totals, grad_inputs = lax.scan(one_sequence, start, (inputs, pre_gate, pre_up, cotangent))
    factor = float(TOKENS) ** (-0.5)
    return (grad_inputs, totals[0] * factor, totals[1] * factor, totals[2] * factor, totals[3] * factor)
```

```python
import jax
import jax.numpy as jnp
from jax import lax
from jax.sharding import PartitionSpec as P


SIDE = 4
HOPS = (1, 3, 2)


def causal_mix(signal, kernel):
    length = signal.shape[0]
    padded = jnp.pad(signal, ((2, 0), (0, 0)))
    return (
        kernel[0] * padded[0:length]
        + kernel[1] * padded[1 : length + 1]
        + kernel[2] * padded[2 : length + 2]
    )


def gated_hidden(gate_pre, up_pre, kernel_gate, kernel_up):
    return jax.nn.gelu(causal_mix(gate_pre, kernel_gate)) * causal_mix(up_pre, kernel_up)


def shift(value, axis, hop):
    ring = range(SIDE)
    if axis == "y":
        return lax.ppermute(value, "fs", [(i, (i + hop) % SIDE) for i in ring])
    if axis == "z":
        pairs = [(z * SIDE + x, (z + hop) % SIDE * SIDE + x) for z in ring for x in ring]
    else:
        pairs = [(z * SIDE + x, z * SIDE + (x + hop) % SIDE) for z in ring for x in ring]
    return lax.ppermute(value, "rep", pairs)


def place(axis):
    if axis == "y":
        return lax.axis_index("fs")
    rep = lax.axis_index("rep")
    return rep // SIDE if axis == "z" else rep % SIDE


def reduce_over(value, axis, dim):
    me = place(axis)
    arrived = [
        shift(lax.dynamic_slice_in_dim(value, (me + hop) % SIDE, 1, dim), axis, hop) for hop in HOPS
    ]
    total = lax.dynamic_slice_in_dim(value, me, 1, dim).astype(jnp.float32)
    for part in arrived:
        total = total + part.astype(jnp.float32)
    return total.astype(jnp.bfloat16)


def gather_over(value, axis, dim):
    me = place(axis)
    arrived = [shift(value, axis, hop) for hop in HOPS]
    lengths = list(value.shape)
    lengths[dim] = SIDE
    result = lax.dynamic_update_slice_in_dim(jnp.zeros(lengths, value.dtype), value, me, dim)
    for hop, part in zip(HOPS, arrived):
        result = lax.dynamic_update_slice_in_dim(result, part, (me + SIDE - hop) % SIDE, dim)
    return result


def sum_over(value, axis):
    arrived = [shift(value, axis, hop) for hop in HOPS]
    return value + arrived[0] + arrived[1] + arrived[2]


def per_device(inputs, pre_gate, pre_up, cotangent, w_gate, w_up, taps_gate, taps_up):
    columns = pre_gate.shape[2]
    reps, shards = lax.axis_size("rep"), lax.axis_size("fs")
    share = w_gate.shape[0] // reps
    tp = lax.axis_index("tp")
    rep = lax.axis_index("rep")
    offset = tp * columns
    swap = [(0, 1), (1, 0)]
    factor = float(pre_gate.shape[1] * reps * shards) ** (-0.5)

    mine = jnp.concatenate(
        [
            lax.dynamic_slice_in_dim(w_gate, rep * share, share, 0),
            lax.dynamic_slice_in_dim(w_up, rep * share, share, 0),
        ],
        axis=1,
    )
    weights = lax.all_gather(mine, ("fs", "rep"), axis=0, tiled=True)

    half = inputs.shape[1]
    own_rows = inputs[0]
    other_rows = lax.ppermute(own_rows, "tp", swap)

    kernel_gate = lax.dynamic_slice_in_dim(taps_gate, offset, columns, 1).astype(jnp.float32)
    kernel_up = lax.dynamic_slice_in_dim(taps_up, offset, columns, 1).astype(jnp.float32)
    _, pullback = jax.vjp(
        gated_hidden,
        pre_gate[0].astype(jnp.float32),
        pre_up[0].astype(jnp.float32),
        kernel_gate,
        kernel_up,
    )
    back_gate, back_up, tap_gate, tap_up = pullback(cotangent[0].astype(jnp.float32))
    stacked = jnp.concatenate([back_gate.astype(jnp.bfloat16), back_up.astype(jnp.bfloat16)], axis=1)

    first = jnp.where(tp == 0, own_rows, other_rows)
    second = jnp.where(tp == 0, other_rows, own_rows)
    whole_rows = jnp.concatenate([first, second], axis=0)
    dims = {"y": 0, "z": 1, "x": 2}
    pieces, start = [], 0
    for width, order in ((1024, "yzx"), (896, "zxy"), (896, "xyz")):
        block = stacked[:, start : start + width]
        start += width
        value = jnp.einsum("nd,nk->dk", whole_rows, block, preferred_element_type=jnp.float32)
        value = value.astype(jnp.bfloat16).reshape(SIDE, SIDE, SIDE, share, width)
        for axis in order:
            value = reduce_over(value, axis, dims[axis])
        pieces.append(value.reshape(share, width))
    piece = jnp.concatenate(pieces, axis=1).reshape(1, 1, share, 2 * columns)
    grads = []
    for part, order in ((piece[..., :columns], "zx"), (piece[..., columns:], "xz")):
        for axis in order:
            part = gather_over(part, axis, "zx".index(axis))
        grads.append(part.reshape(reps * share, columns).astype(jnp.float32) * factor)

    taps = jnp.concatenate([tap_gate, tap_up], axis=0)
    for axis in "yzx":
        taps = sum_over(taps, axis)
    taps = taps * factor
    other_taps = lax.ppermute(taps, "tp", swap)
    taps = jnp.where(
        tp == 0,
        jnp.concatenate([taps, other_taps], axis=1),
        jnp.concatenate([other_taps, taps], axis=1),
    )

    partial = jnp.einsum("nk,dk->nd", stacked, weights, preferred_element_type=jnp.float32)
    partial = partial.astype(jnp.bfloat16)
    keep = lax.dynamic_slice_in_dim(partial, tp * half, half, 0)
    send = lax.dynamic_slice_in_dim(partial, (1 - tp) * half, half, 0)
    got = lax.ppermute(send, "tp", swap)
    grad_inputs = (keep.astype(jnp.float32) + got.astype(jnp.float32)).astype(jnp.bfloat16)[None]
    return (grad_inputs, grads[0], grads[1], taps[:3], taps[3:])


def solution(mesh):
    placed = (
        P(("rep", "fs"), "tp", None),
        P(("rep", "fs"), None, "tp"),
        P(("rep", "fs"), None, "tp"),
        P(("rep", "fs"), None, "tp"),
        P("fs", "tp"),
        P("fs", "tp"),
        P(),
        P(),
    )
    return jax.shard_map(
        per_device,
        mesh=mesh,
        in_specs=placed,
        out_specs=(P(("rep", "fs"), "tp", None), P("fs", "tp"), P("fs", "tp"), P(), P()),
        check_vma=False,
    )
```

```python
import functools

import jax
import jax.numpy as jnp
from jax import lax
from jax.experimental import pallas as pl
from jax.experimental.pallas import tpu as pltpu
from jax.sharding import PartitionSpec as P


SIDE = 4
HOPS = (1, 3, 2)
LANES = 128
CHUNK = 32
HALO = 8
GROUPS = ((6, "zx"), (5, "xz"))
DIMS = {"y": 0, "z": 1, "x": 2}


def shift(value, axis, hop):
    ring = range(SIDE)
    if axis == "y":
        return lax.ppermute(value, "fs", [(i, (i + hop) % SIDE) for i in ring])
    if axis == "z":
        pairs = [(z * SIDE + x, (z + hop) % SIDE * SIDE + x) for z in ring for x in ring]
    else:
        pairs = [(z * SIDE + x, z * SIDE + (x + hop) % SIDE) for z in ring for x in ring]
    return lax.ppermute(value, "rep", pairs)


def place(axis):
    if axis == "y":
        return lax.axis_index("fs")
    rep = lax.axis_index("rep")
    return rep // SIDE if axis == "z" else rep % SIDE


def parts_for(value, extra, axis):
    me, dim, width = place(axis), DIMS[axis], value.shape[-1]
    sent = []
    for hop in HOPS:
        part = lax.dynamic_slice_in_dim(value, (me + hop) % SIDE, 1, dim).reshape(-1, width)
        sent.append(part if extra is None else jnp.concatenate([part, extra], axis=0))
    return sent, (lax.dynamic_slice_in_dim(value, me, 1, dim), extra)


def exchange(sent, axis):
    return [shift(part, axis, hop) for hop, part in zip(HOPS, sent)]


def four(own, one, three, two):
    return (own + two) + (one + three)


def two_parts(taps):
    high = lax.reduce_precision(taps, 8, 7)
    return high.astype(jnp.bfloat16), (taps - high).astype(jnp.bfloat16)


def add_up(kept, arrived):
    own, extra = kept
    width, count = own.shape[-1], own.size // own.shape[-1]
    heads = [own.reshape(count, width)] + [part[:count] for part in arrived]
    total = four(*[head.astype(jnp.float32) for head in heads])
    tails = None
    if extra is not None:
        tails = [extra] + [part[count:] for part in arrived]
    return total.astype(jnp.bfloat16).reshape(own.shape), tails


def gather_over(value, axis):
    one, three, two = exchange([value] * 3, axis)
    turn = (place(axis) + SIDE - jnp.arange(SIDE)) % SIDE
    turn = turn.reshape((SIDE,) + (1,) * value.ndim)
    return jnp.where(
        turn == 0, value, jnp.where(turn == 1, one, jnp.where(turn == 2, two, three))
    )


def backward_kernel(tp_ref, gate_ref, up_ref, cot_ref, tap_gate_ref, tap_up_ref, *rest):
    group_ref, stacked_ref, sums_ref, gate_pad, up_pad = rest[-5:]
    length = gate_ref.shape[0]
    zeros = jnp.zeros((HALO, LANES), jnp.float32)
    gate_pad[0:HALO, :] = zeros
    up_pad[0:HALO, :] = zeros
    gate_pad[HALO : HALO + length, :] = gate_ref[...].astype(jnp.float32)
    up_pad[HALO : HALO + length, :] = up_ref[...].astype(jnp.float32)
    kg = tap_gate_ref[...].astype(jnp.float32)
    ku = tap_up_ref[...].astype(jnp.float32)
    kg = [jnp.broadcast_to(kg[j : j + 1], (CHUNK, LANES)) for j in range(3)]
    ku = [jnp.broadcast_to(ku[j : j + 1], (CHUNK, LANES)) for j in range(3)]
    root = 0.7978845608028654
    count = length // CHUNK

    def delayed(pad, row):
        rows = pad[pl.ds(row, CHUNK + HALO), :]
        return [pltpu.roll(rows, 2, 0)[HALO:], pltpu.roll(rows, 1, 0)[HALO:], rows[HALO:]]

    def advanced(now, later, kernel):
        rows = jnp.concatenate([now, later], axis=0)
        one = pltpu.roll(rows, CHUNK + HALO - 1, 0)[:CHUNK]
        two = pltpu.roll(rows, CHUNK + HALO - 2, 0)[:CHUNK]
        return kernel[2] * now + kernel[1] * one + kernel[0] * two

    def folded(product):
        return jnp.sum(product.reshape(CHUNK // 8, 8, LANES), axis=0)

    def step(index, carry):
        later_gate, later_up, sums = carry
        row = pl.multiple_of((count - 1 - index) * CHUNK, CHUNK)
        gates = delayed(gate_pad, row)
        ups = delayed(up_pad, row)
        cot = cot_ref[pl.ds(row, CHUNK), :].astype(jnp.float32)
        v = kg[0] * gates[0] + kg[1] * gates[1] + kg[2] * gates[2]
        mixed_up = ku[0] * ups[0] + ku[1] * ups[1] + ku[2] * ups[2]
        square = v * v
        bent = jnp.tanh(v * (root + (root * 0.044715) * square))
        rise = 0.5 + 0.5 * bent
        slope = rise + (0.5 * v) * (1.0 - bent * bent) * (root + (3.0 * root * 0.044715) * square)
        back_gate = cot * mixed_up * slope
        back_up = cot * (v * rise)
        out_gate = advanced(back_gate, later_gate, kg).astype(jnp.bfloat16)
        out_up = advanced(back_up, later_up, ku).astype(jnp.bfloat16)
        for ref in (group_ref, stacked_ref):
            ref[pl.ds(row, CHUNK), 0:LANES] = out_gate
            ref[pl.ds(row, CHUNK), LANES : 2 * LANES] = out_up
        products = [back_gate * g for g in gates] + [back_up * u for u in ups]
        sums = tuple(s + folded(p) for s, p in zip(sums, products))
        return back_gate[:HALO], back_up[:HALO], sums

    start = (zeros, zeros, (zeros,) * 6)
    sums = lax.fori_loop(0, count, step, start)[2]
    rows = [jnp.sum(s, axis=0, keepdims=True) for s in sums]
    sums_ref[...] = jnp.concatenate(rows + [jnp.zeros((2, LANES), jnp.float32)], axis=0)


def backward(tp, pre_gate, pre_up, cotangent, taps_gate, taps_up, first, blocks, stacked):
    length, columns = pre_gate.shape
    total = columns // LANES
    wide = pl.BlockSpec((length, LANES), lambda j, t: (0, first + j))
    taps = pl.BlockSpec((3, LANES), lambda j, t: (0, t[0] * total + first + j))
    operands = [tp, pre_gate, pre_up, cotangent, taps_gate, taps_up]
    in_specs = [wide, wide, wide, taps, taps]
    aliases = {}
    if stacked is not None:
        aliases = {len(operands): 1}
        operands.append(stacked)
        in_specs.append(pl.BlockSpec(memory_space=pl.ANY))
    return pl.pallas_call(
        backward_kernel,
        grid_spec=pltpu.PrefetchScalarGridSpec(
            num_scalar_prefetch=1,
            grid=(blocks,),
            in_specs=in_specs,
            out_specs=[
                pl.BlockSpec((length, 2 * LANES), lambda j, t: (0, j)),
                pl.BlockSpec((length, 2 * LANES), lambda j, t: (0, first + j)),
                pl.BlockSpec((8, LANES), lambda j, t: (0, j)),
            ],
            scratch_shapes=[pltpu.VMEM((length + HALO, LANES), jnp.float32)] * 2,
        ),
        out_shape=[
            jax.ShapeDtypeStruct((length, blocks * 2 * LANES), jnp.bfloat16),
            jax.ShapeDtypeStruct((length, 2 * columns), jnp.bfloat16),
            jax.ShapeDtypeStruct((8, blocks * LANES), jnp.float32),
        ],
        input_output_aliases=aliases,
        cost_estimate=pl.CostEstimate(
            flops=2000 * length * LANES * blocks,
            bytes_accessed=length * LANES * blocks * 14,
            transcendentals=length * LANES * blocks,
        ),
        name="backward",
    )(*operands)


def weave_kernel(gate_ref, up_ref, out_ref):
    for block in range(gate_ref.shape[1] // LANES):
        columns = slice(block * LANES, (block + 1) * LANES)
        out_ref[:, 2 * block * LANES : (2 * block + 1) * LANES] = gate_ref[:, columns]
        out_ref[:, (2 * block + 1) * LANES : (2 * block + 2) * LANES] = up_ref[:, columns]


def weave(gate, up):
    rows, columns = gate.shape
    narrow = pl.BlockSpec((rows // SIDE, columns), lambda j: (j, 0))
    return pl.pallas_call(
        weave_kernel,
        grid=(SIDE,),
        in_specs=[narrow, narrow],
        out_specs=pl.BlockSpec((rows // SIDE, 2 * columns), lambda j: (j, 0)),
        out_shape=jax.ShapeDtypeStruct((rows, 2 * columns), gate.dtype),
        cost_estimate=pl.CostEstimate(
            flops=100 * rows * columns, bytes_accessed=8 * rows * columns, transcendentals=0
        ),
        name="weave",
    )(gate, up)


def join_kernel(place_ref, *refs):
    kept, got, out_ref, sums, sems = refs[:4], refs[4:8], refs[8], refs[9], refs[10]
    width = sums.shape[-1]
    copies = []
    for number, hop in enumerate((0,) + HOPS):
        total = kept[number][...].astype(jnp.float32) + got[number][...].astype(jnp.float32)
        sums[number] = total.astype(jnp.bfloat16)
        source = lax.rem(place_ref[0] + SIDE - hop, SIDE)
        target = out_ref.at[:, pl.ds(pl.multiple_of(source * width, width), width)]
        copies.append(pltpu.make_async_copy(sums.at[number], target, sems.at[number]))
        if number:
            copies[number - 1].start()
    copies[-1].start()
    for copy in copies:
        copy.wait()


def join(place_y, kept, got):
    rows, width = kept[0].shape
    return pl.pallas_call(
        join_kernel,
        in_specs=[pl.BlockSpec(memory_space=pltpu.SMEM)]
        + [pl.BlockSpec(memory_space=pltpu.VMEM)] * (2 * SIDE),
        out_specs=pl.BlockSpec(memory_space=pl.ANY),
        out_shape=jax.ShapeDtypeStruct((rows, SIDE * width), jnp.bfloat16),
        scratch_shapes=[
            pltpu.VMEM((SIDE, rows, width), jnp.bfloat16),
            pltpu.SemaphoreType.DMA((SIDE,)),
        ],
        cost_estimate=pl.CostEstimate(
            flops=400 * rows * width, bytes_accessed=24 * rows * width, transcendentals=0
        ),
        name="join",
    )(place_y, *kept, *got)


def finish_kernel(plan, factor, places, *refs):
    count = sum(len(lists) for _, _, lists in plan)
    pieces, outs = refs[:count], refs[count : count + 2]
    halves, sems = refs[count + 2 : -1], refs[-1]
    copies, number = [], 0

    def begin(index):
        for copy in copies[2 * index : 2 * index + 2]:
            copy.start()

    for low, axis, hops in plan:
        me = places[0] if axis == "z" else places[1]
        for hop in hops:
            piece, half = pieces[number], halves[number]
            width = piece.shape[-1] // 2
            for block in range(width // LANES):
                values = piece[:, :, 2 * block * LANES : 2 * (block + 1) * LANES]
                values = values.astype(jnp.float32) * factor
                half[0, :, :, block * LANES : (block + 1) * LANES] = values[:, :, :LANES]
                half[1, :, :, block * LANES : (block + 1) * LANES] = values[:, :, LANES:]
            source = lax.rem(me + SIDE - hop, SIDE)
            for side in range(2):
                columns = pl.ds(low * LANES, width)
                if axis == "z":
                    target = outs[side].at[source, :, :, columns]
                else:
                    target = outs[side].at[:, source, :, columns]
                copies.append(pltpu.make_async_copy(half.at[side], target, sems.at[number, side]))
            if number:
                begin(number - 1)
            number += 1
    begin(number - 1)
    for copy in copies:
        copy.wait()


def finish(places, plan, pieces, columns, factor):
    share = pieces[0].shape[1]
    out = jax.ShapeDtypeStruct((SIDE, SIDE, share, columns), jnp.float32)
    size = SIDE * SIDE * share * columns
    return pl.pallas_call(
        functools.partial(finish_kernel, plan, factor),
        in_specs=[pl.BlockSpec(memory_space=pltpu.SMEM)]
        + [pl.BlockSpec(memory_space=pltpu.VMEM)] * len(pieces),
        out_specs=[pl.BlockSpec(memory_space=pl.ANY)] * 2,
        out_shape=[out, out],
        scratch_shapes=[
            pltpu.VMEM((2, SIDE, share, p.shape[-1] // 2), jnp.float32) for p in pieces
        ]
        + [pltpu.SemaphoreType.DMA((len(pieces), 2))],
        cost_estimate=pl.CostEstimate(
            flops=200 * size, bytes_accessed=12 * size, transcendentals=0
        ),
        name="finish",
    )(places, *pieces)


def layer(inputs, pre_gate, pre_up, cotangent, w_gate, w_up, taps_gate, taps_up):
    columns = pre_gate.shape[2]
    reps, shards = lax.axis_size("rep"), lax.axis_size("fs")
    share = w_gate.shape[0] // reps
    tp = lax.axis_index("tp")
    swap = [(0, 1), (1, 0)]
    factor = float(pre_gate.shape[1] * reps * shards) ** (-0.5)

    shard = weave(w_gate, w_up)
    below, above = shift(shard, "y", 1), shift(shard, "y", SIDE - 1)
    middle_row = shard.shape[0] // 2
    opposite = [shift(below[:middle_row], "y", 1), shift(above[middle_row:], "y", SIDE - 1)]

    half = inputs.shape[1]
    own_rows = inputs[0]
    other_rows = lax.ppermute(own_rows, "tp", swap)
    first = jnp.where(tp == 0, own_rows, other_rows)
    second = jnp.where(tp == 0, other_rows, own_rows)
    whole_rows = jnp.concatenate([first, second], axis=0)

    where = jnp.full((1,), tp, jnp.int32)
    stacked, low, groups, tap_sums = None, 0, [], []
    for blocks, _ in GROUPS:
        group, stacked, taps = backward(
            where, pre_gate[0], pre_up[0], cotangent[0], taps_gate, taps_up, low, blocks, stacked
        )
        low += blocks
        groups.append(group)
        tap_sums.append(taps)
    taps = jnp.concatenate(tap_sums, axis=1)
    wide = groups[0].shape[1]
    taps = jnp.pad(taps, ((0, 0), (0, wide - columns)))
    extra = jnp.concatenate(two_parts(taps), axis=0)

    begun = []
    for group, (_, order) in zip(groups, GROUPS):
        value = jnp.einsum("nd,nk->dk", whole_rows, group, preferred_element_type=jnp.float32)
        value = value.astype(jnp.bfloat16).reshape(SIDE, SIDE, SIDE, share, group.shape[1])
        sent, kept = parts_for(value, extra, order[0])
        extra = None
        begun.append((kept, exchange(sent, order[0])))

    lower = lax.optimization_barrier(lax.optimization_barrier(tp) == 0)
    upper = lax.optimization_barrier(lax.optimization_barrier(tp) == 1)

    def folded(tails):
        return four(*[t[:8].astype(jnp.float32) + t[8:].astype(jnp.float32) for t in tails])

    middle = []
    for (kept, arrived), (_, order) in zip(begun, GROUPS):
        value, tails = add_up(kept, arrived)
        extra = None if tails is None else jnp.concatenate(two_parts(folded(tails)), axis=0)
        sent, kept = parts_for(value, extra, order[1])
        middle.append((kept, exchange(sent, order[1])))

    values = []
    for kept, arrived in middle:
        value, tails = add_up(kept, arrived)
        values.append(value.reshape(SIDE, 1, 1, share, value.shape[-1]))
        if tails is not None:
            taps = folded(tails)[:, :columns]
    both = jnp.concatenate(values, axis=-1)
    sent, kept = parts_for(both, jnp.concatenate(two_parts(taps), axis=1), "y")
    arrived = exchange(sent, "y")
    value, tails = add_up(kept, arrived)
    value = value.reshape(share, 2 * columns)
    taps = four(
        *[t[:, :columns].astype(jnp.float32) + t[:, columns:].astype(jnp.float32) for t in tails]
    )

    low, plan, pieces, parts = 0, [], [], []
    for blocks, order in GROUPS:
        part = value[:, 2 * LANES * low : 2 * LANES * (low + blocks)]
        parts.append(gather_over(part, order[0]))
        plan.append((low, order[1], (0,) + HOPS))
        low += blocks
    for part, (_, order) in zip(parts, GROUPS):
        pieces += [part] + exchange([part] * 3, order[1])
    places = jnp.stack([place("z"), place("x")]).astype(jnp.int32)
    grads = finish(places, tuple(plan), pieces, columns, factor)
    grads = [g.reshape(reps * share, columns) for g in grads]

    taps = taps * factor
    other_taps = lax.ppermute(taps, "tp", swap)
    grad_taps = [
        jnp.concatenate([jnp.where(ours, t, o), jnp.where(ours, o, t)], axis=1)
        for ours, t, o in (
            (lower, taps[:3], other_taps[:3]),
            (jnp.logical_not(upper), taps[3:6], other_taps[3:6]),
        )
    ]

    def project(w):
        result = jnp.einsum("nk,dk->nd", stacked, w, preferred_element_type=jnp.float32)
        return result.astype(jnp.bfloat16)

    partials = [project(shard), project(below), project(above)]
    partials.append(jnp.concatenate([project(w) for w in opposite], axis=1))
    away = [lax.dynamic_slice_in_dim(p, (1 - tp) * half, half, 0) for p in partials]
    kept = [lax.dynamic_slice_in_dim(p, tp * half, half, 0) for p in partials]
    got = [lax.ppermute(p, "tp", swap) for p in away]
    grad_inputs = join(jnp.full((1,), place("y"), jnp.int32), kept, got)[None]
    return (grad_inputs, grads[0], grads[1], grad_taps[0], grad_taps[1])


def solution(mesh):
    placed = (
        P(("rep", "fs"), "tp", None),
        P(("rep", "fs"), None, "tp"),
        P(("rep", "fs"), None, "tp"),
        P(("rep", "fs"), None, "tp"),
        P("fs", "tp"),
        P("fs", "tp"),
        P(),
        P(),
    )
    return jax.shard_map(
        layer,
        mesh=mesh,
        in_specs=placed,
        out_specs=(P(("rep", "fs"), "tp", None), P("fs", "tp"), P("fs", "tp"), P(), P()),
        check_vma=False,
    )
```

```python
import functools

import jax
import jax.numpy as jnp
from jax import lax
from jax.experimental import pallas as pl
from jax.experimental.pallas import tpu as pltpu
from jax.sharding import PartitionSpec as P


SIDE = 4
HOPS = (1, 3, 2)
LANES = 128
CHUNK = 32
HALO = 8
GROUPS = ((7, "zx"), (4, "xz"))
GATHERS = ((6, "zx"), (5, "xz"))
DIMS = {"y": 0, "z": 1, "x": 2}


def shift(value, axis, hop):
    ring = range(SIDE)
    if axis == "y":
        return lax.ppermute(value, "fs", [(i, (i + hop) % SIDE) for i in ring])
    if axis == "z":
        pairs = [(z * SIDE + x, (z + hop) % SIDE * SIDE + x) for z in ring for x in ring]
    else:
        pairs = [(z * SIDE + x, z * SIDE + (x + hop) % SIDE) for z in ring for x in ring]
    return lax.ppermute(value, "rep", pairs)


def place(axis):
    if axis == "y":
        return lax.axis_index("fs")
    rep = lax.axis_index("rep")
    return rep // SIDE if axis == "z" else rep % SIDE


def parts_for(value, extra, axis):
    me, dim, width = place(axis), DIMS[axis], value.shape[-1]
    sent = []
    for hop in HOPS:
        part = lax.dynamic_slice_in_dim(value, (me + hop) % SIDE, 1, dim).reshape(-1, width)
        sent.append(part if extra is None else jnp.concatenate([part, extra], axis=0))
    return sent, (lax.dynamic_slice_in_dim(value, me, 1, dim), extra)


def exchange(sent, axis):
    return [shift(part, axis, hop) for hop, part in zip(HOPS, sent)]


def four(own, one, three, two):
    return (own + two) + (one + three)


def tap_kernel(columns, width, scale, *refs):
    out_ref, values = refs[-1], []
    for ref in refs[:-1]:
        rows = ref[...].astype(jnp.float32)
        if rows.shape[0] > 8:
            cut = rows.shape[0] // 2
            both = rows[:cut] + rows[cut:]
            pieces = [both[k : k + 8] for k in range(0, cut, 8)]
            values.append(jnp.concatenate(pieces, axis=1)[:, :columns])
        elif rows.shape[1] == 2 * columns:
            values.append(rows[:, :columns] + rows[:, columns:])
        else:
            values.append(rows)
    total = four(*values) if len(values) == SIDE else jnp.concatenate(values, axis=1)
    if scale is not None:
        out_ref[...] = total * scale
        return
    high = total.astype(jnp.bfloat16).astype(jnp.float32)
    parts = [high, total - high]
    if width == 2 * columns:
        out_ref[...] = jnp.concatenate(parts, axis=1).astype(jnp.bfloat16)
        return
    count = out_ref.shape[0] // 16
    if count * width > columns:
        blank = jnp.zeros((8, count * width - columns), jnp.float32)
        parts = [jnp.concatenate([part, blank], axis=1) for part in parts]
    cuts = [part[:, k * width : (k + 1) * width] for part in parts for k in range(count)]
    out_ref[...] = jnp.concatenate(cuts, axis=0).astype(jnp.bfloat16)


def tap_rows(tails, rows, columns, width, scale=None):
    count = 8 if width == 2 * columns else 16 * (-(-columns // width))
    out = (8, columns) if scale is not None else (count, width)
    kind = jnp.float32 if scale is not None else jnp.bfloat16

    def spec(tail):
        last = tail.shape[0] // rows - 1
        return pl.BlockSpec((rows, tail.shape[1]), lambda j: (last, 0))

    return pl.pallas_call(
        functools.partial(tap_kernel, columns, width, scale),
        grid=(1,),
        in_specs=[spec(tail) for tail in tails],
        out_specs=pl.BlockSpec(out, lambda j: (0, 0)),
        out_shape=jax.ShapeDtypeStruct(out, kind),
        cost_estimate=pl.CostEstimate(flops=100000, bytes_accessed=500000, transcendentals=0),
        name="tap_rows",
    )(*tails)


def add_up(kept, arrived):
    own, extra = kept
    width, count = own.shape[-1], own.size // own.shape[-1]
    heads = [own.reshape(count, width)] + [part[:count] for part in arrived]
    total = four(*[head.astype(jnp.float32) for head in heads])
    tails = None
    if extra is not None:
        tails = [extra] + arrived
    return total.astype(jnp.bfloat16).reshape(own.shape), tails


def relay_out(value, extra, axis):
    me, dim, width = place(axis), DIMS[axis], value.shape[-1]
    own, right, opposite, left = [
        lax.dynamic_slice_in_dim(value, (me + hop) % SIDE, 1, dim).reshape(-1, width)
        for hop in range(SIDE)
    ]
    cut = own.shape[0] // 2
    tail = [] if extra is None else [extra]
    upward = jnp.concatenate([opposite[:cut], right[cut:]] + tail, axis=0)
    downward = jnp.concatenate([opposite[cut:], left[:cut]] + tail, axis=0)
    return upward, downward, (own, right[:cut], left[cut:], extra)


def relay_on(kept, arrived):
    _, right, left, extra = kept
    cut = right.shape[0]
    below, above = arrived
    upward = (right.astype(jnp.float32) + below[:cut].astype(jnp.float32)).astype(jnp.bfloat16)
    downward = (left.astype(jnp.float32) + above[:cut].astype(jnp.float32)).astype(jnp.bfloat16)
    if extra is not None:
        upward = jnp.concatenate([upward, below[2 * cut :]], axis=0)
    return upward, downward


def relay_sum(kept, arrived, later):
    own, right, _, extra = kept
    cut = right.shape[0]
    below, above = arrived
    top = own[:cut].astype(jnp.float32) + above[cut : 2 * cut].astype(jnp.float32)
    bottom = own[cut:].astype(jnp.float32) + below[cut : 2 * cut].astype(jnp.float32)
    top = top + later[0][:cut].astype(jnp.float32)
    bottom = bottom + later[1].astype(jnp.float32)
    total = jnp.concatenate([top.astype(jnp.bfloat16), bottom.astype(jnp.bfloat16)], axis=0)
    tails = None
    if extra is not None:
        tails = [extra, below, above, later[0]]
    return total, tails


def gather_over(value, axis):
    one, three, two = exchange([value] * 3, axis)
    turn = (place(axis) + SIDE - jnp.arange(SIDE)) % SIDE
    turn = turn.reshape((SIDE,) + (1,) * value.ndim)
    return jnp.where(
        turn == 0, value, jnp.where(turn == 1, one, jnp.where(turn == 2, two, three))
    )


def backward_kernel(tp_ref, gate_ref, up_ref, cot_ref, tap_gate_ref, tap_up_ref, *rest):
    group_ref, stacked_ref, sums_ref, gate_pad, up_pad = rest[-5:]
    length = gate_ref.shape[0]
    zeros = jnp.zeros((HALO, LANES), jnp.float32)
    gate_pad[0:HALO, :] = zeros
    up_pad[0:HALO, :] = zeros
    gate_pad[HALO : HALO + length, :] = gate_ref[...].astype(jnp.float32)
    up_pad[HALO : HALO + length, :] = up_ref[...].astype(jnp.float32)
    kg = tap_gate_ref[...].astype(jnp.float32)
    ku = tap_up_ref[...].astype(jnp.float32)
    kg = [jnp.broadcast_to(kg[j : j + 1], (CHUNK, LANES)) for j in range(3)]
    ku = [jnp.broadcast_to(ku[j : j + 1], (CHUNK, LANES)) for j in range(3)]
    root = 0.7978845608028654
    count = length // CHUNK

    def delayed(pad, row):
        rows = pad[pl.ds(row, CHUNK + HALO), :]
        return [pltpu.roll(rows, 2, 0)[HALO:], pltpu.roll(rows, 1, 0)[HALO:], rows[HALO:]]

    def advanced(now, later, kernel):
        rows = jnp.concatenate([now, later], axis=0)
        one = pltpu.roll(rows, CHUNK + HALO - 1, 0)[:CHUNK]
        two = pltpu.roll(rows, CHUNK + HALO - 2, 0)[:CHUNK]
        return kernel[2] * now + kernel[1] * one + kernel[0] * two

    def folded(product):
        return jnp.sum(product.reshape(CHUNK // 8, 8, LANES), axis=0)

    def step(index, carry):
        later_gate, later_up, sums = carry
        row = pl.multiple_of((count - 1 - index) * CHUNK, CHUNK)
        gates = delayed(gate_pad, row)
        ups = delayed(up_pad, row)
        cot = cot_ref[pl.ds(row, CHUNK), :].astype(jnp.float32)
        v = kg[0] * gates[0] + kg[1] * gates[1] + kg[2] * gates[2]
        mixed_up = ku[0] * ups[0] + ku[1] * ups[1] + ku[2] * ups[2]
        square = v * v
        bent = jnp.tanh(v * (root + (root * 0.044715) * square))
        rise = 0.5 + 0.5 * bent
        slope = rise + (0.5 * v) * (1.0 - bent * bent) * (root + (3.0 * root * 0.044715) * square)
        back_gate = cot * mixed_up * slope
        back_up = cot * (v * rise)
        out_gate = advanced(back_gate, later_gate, kg).astype(jnp.bfloat16)
        out_up = advanced(back_up, later_up, ku).astype(jnp.bfloat16)
        for ref in (group_ref, stacked_ref):
            ref[pl.ds(row, CHUNK), 0:LANES] = out_gate
            ref[pl.ds(row, CHUNK), LANES : 2 * LANES] = out_up
        products = [back_gate * g for g in gates] + [back_up * u for u in ups]
        sums = tuple(s + folded(p) for s, p in zip(sums, products))
        return back_gate[:HALO], back_up[:HALO], sums

    start = (zeros, zeros, (zeros,) * 6)
    sums = lax.fori_loop(0, count, step, start)[2]
    rows = [jnp.sum(s, axis=0, keepdims=True) for s in sums]
    sums_ref[...] = jnp.concatenate(rows + [jnp.zeros((2, LANES), jnp.float32)], axis=0)


def backward(tp, pre_gate, pre_up, cotangent, taps_gate, taps_up, first, blocks, stacked):
    length, columns = pre_gate.shape
    total = columns // LANES
    wide = pl.BlockSpec((length, LANES), lambda j, t: (0, first + j))
    taps = pl.BlockSpec((3, LANES), lambda j, t: (0, t[0] * total + first + j))
    operands = [tp, pre_gate, pre_up, cotangent, taps_gate, taps_up]
    in_specs = [wide, wide, wide, taps, taps]
    aliases = {}
    if stacked is not None:
        aliases = {len(operands): 1}
        operands.append(stacked)
        in_specs.append(pl.BlockSpec(memory_space=pl.ANY))
    return pl.pallas_call(
        backward_kernel,
        grid_spec=pltpu.PrefetchScalarGridSpec(
            num_scalar_prefetch=1,
            grid=(blocks,),
            in_specs=in_specs,
            out_specs=[
                pl.BlockSpec((length, 2 * LANES), lambda j, t: (0, j)),
                pl.BlockSpec((length, 2 * LANES), lambda j, t: (0, first + j)),
                pl.BlockSpec((8, LANES), lambda j, t: (0, j)),
            ],
            scratch_shapes=[pltpu.VMEM((length + HALO, LANES), jnp.float32)] * 2,
        ),
        out_shape=[
            jax.ShapeDtypeStruct((length, blocks * 2 * LANES), jnp.bfloat16),
            jax.ShapeDtypeStruct((length, 2 * columns), jnp.bfloat16),
            jax.ShapeDtypeStruct((8, blocks * LANES), jnp.float32),
        ],
        input_output_aliases=aliases,
        cost_estimate=pl.CostEstimate(
            flops=2000 * length * LANES * blocks,
            bytes_accessed=length * LANES * blocks * 14,
            transcendentals=length * LANES * blocks,
        ),
        name="backward",
    )(*operands)


def weave_kernel(gate_ref, up_ref, out_ref):
    for block in range(gate_ref.shape[1] // LANES):
        columns = slice(block * LANES, (block + 1) * LANES)
        out_ref[:, 2 * block * LANES : (2 * block + 1) * LANES] = gate_ref[:, columns]
        out_ref[:, (2 * block + 1) * LANES : (2 * block + 2) * LANES] = up_ref[:, columns]


def weave(gate, up):
    rows, columns = gate.shape
    narrow = pl.BlockSpec((rows // SIDE, columns), lambda j: (j, 0))
    return pl.pallas_call(
        weave_kernel,
        grid=(SIDE,),
        in_specs=[narrow, narrow],
        out_specs=pl.BlockSpec((rows // SIDE, 2 * columns), lambda j: (j, 0)),
        out_shape=jax.ShapeDtypeStruct((rows, 2 * columns), gate.dtype),
        cost_estimate=pl.CostEstimate(
            flops=100 * rows * columns, bytes_accessed=8 * rows * columns, transcendentals=0
        ),
        name="weave",
    )(gate, up)


def join_kernel(place_ref, *refs):
    kept, got, out_ref, sums, sems = refs[:4], refs[4:8], refs[8], refs[9], refs[10]
    width = sums.shape[-1]
    copies = []
    for number, hop in enumerate((0,) + HOPS):
        total = kept[number][...].astype(jnp.float32) + got[number][...].astype(jnp.float32)
        sums[number] = total.astype(jnp.bfloat16)
        source = lax.rem(place_ref[0] + SIDE - hop, SIDE)
        target = out_ref.at[:, pl.ds(pl.multiple_of(source * width, width), width)]
        copies.append(pltpu.make_async_copy(sums.at[number], target, sems.at[number]))
        if number:
            copies[number - 1].start()
    copies[-1].start()
    for copy in copies:
        copy.wait()


def join(place_y, kept, got):
    rows, width = kept[0].shape
    return pl.pallas_call(
        join_kernel,
        in_specs=[pl.BlockSpec(memory_space=pltpu.SMEM)]
        + [pl.BlockSpec(memory_space=pltpu.VMEM)] * (2 * SIDE),
        out_specs=pl.BlockSpec(memory_space=pl.ANY),
        out_shape=jax.ShapeDtypeStruct((rows, SIDE * width), jnp.bfloat16),
        scratch_shapes=[
            pltpu.VMEM((SIDE, rows, width), jnp.bfloat16),
            pltpu.SemaphoreType.DMA((SIDE,)),
        ],
        cost_estimate=pl.CostEstimate(
            flops=400 * rows * width, bytes_accessed=24 * rows * width, transcendentals=0
        ),
        name="join",
    )(place_y, *kept, *got)


def finish_kernel(plan, factor, places, *refs):
    count = sum(len(lists) for _, _, lists in plan)
    pieces, outs = refs[:count], refs[count : count + 2]
    halves, sems = refs[count + 2 : -1], refs[-1]
    copies, number = [], 0

    def begin(index):
        for copy in copies[2 * index : 2 * index + 2]:
            copy.start()

    for low, axis, hops in plan:
        me = places[0] if axis == "z" else places[1]
        for hop in hops:
            piece, half = pieces[number], halves[number]
            width = piece.shape[-1] // 2
            for block in range(width // LANES):
                values = piece[:, :, 2 * block * LANES : 2 * (block + 1) * LANES]
                values = values.astype(jnp.float32) * factor
                half[0, :, :, block * LANES : (block + 1) * LANES] = values[:, :, :LANES]
                half[1, :, :, block * LANES : (block + 1) * LANES] = values[:, :, LANES:]
            source = lax.rem(me + SIDE - hop, SIDE)
            for side in range(2):
                columns = pl.ds(low * LANES, width)
                if axis == "z":
                    target = outs[side].at[source, :, :, columns]
                else:
                    target = outs[side].at[:, source, :, columns]
                copies.append(pltpu.make_async_copy(half.at[side], target, sems.at[number, side]))
            if number:
                begin(number - 1)
            number += 1
    begin(number - 1)
    for copy in copies:
        copy.wait()


def finish(places, plan, pieces, columns, factor):
    share = pieces[0].shape[1]
    out = jax.ShapeDtypeStruct((SIDE, SIDE, share, columns), jnp.float32)
    size = SIDE * SIDE * share * columns
    return pl.pallas_call(
        functools.partial(finish_kernel, plan, factor),
        in_specs=[pl.BlockSpec(memory_space=pltpu.SMEM)]
        + [pl.BlockSpec(memory_space=pltpu.VMEM)] * len(pieces),
        out_specs=[pl.BlockSpec(memory_space=pl.ANY)] * 2,
        out_shape=[out, out],
        scratch_shapes=[
            pltpu.VMEM((2, SIDE, share, p.shape[-1] // 2), jnp.float32) for p in pieces
        ]
        + [pltpu.SemaphoreType.DMA((len(pieces), 2))],
        cost_estimate=pl.CostEstimate(
            flops=200 * size, bytes_accessed=12 * size, transcendentals=0
        ),
        name="finish",
    )(places, *pieces)


def layer(inputs, pre_gate, pre_up, cotangent, w_gate, w_up, taps_gate, taps_up):
    columns = pre_gate.shape[2]
    reps, shards = lax.axis_size("rep"), lax.axis_size("fs")
    share = w_gate.shape[0] // reps
    tp = lax.axis_index("tp")
    swap = [(0, 1), (1, 0)]
    factor = float(pre_gate.shape[1] * reps * shards) ** (-0.5)

    shard = weave(w_gate, w_up)
    below, above = shift(shard, "y", 1), shift(shard, "y", SIDE - 1)
    middle_row = shard.shape[0] // 2
    opposite = [shift(below[:middle_row], "y", 1), shift(above[middle_row:], "y", SIDE - 1)]

    half = inputs.shape[1]
    own_rows = inputs[0]
    other_rows = lax.ppermute(own_rows, "tp", swap)
    first = jnp.where(tp == 0, own_rows, other_rows)
    second = jnp.where(tp == 0, other_rows, own_rows)
    whole_rows = jnp.concatenate([first, second], axis=0)

    where = jnp.full((1,), tp, jnp.int32)
    stacked, low, tap_sums, begun, extra = None, 0, [], [], None
    for number, (blocks, order) in enumerate(GROUPS):
        group, stacked, taps = backward(
            where, pre_gate[0], pre_up[0], cotangent[0], taps_gate, taps_up, low, blocks, stacked
        )
        low += blocks
        tap_sums.append(taps)
        width = group.shape[1]
        if number == len(GROUPS) - 1:
            extra = tap_rows(tap_sums, 8, columns, width)
            tap_count = extra.shape[0]
        value = jnp.einsum("nd,nk->dk", whole_rows, group, preferred_element_type=jnp.float32)
        value = value.astype(jnp.bfloat16).reshape(SIDE, SIDE, SIDE, share, width)
        upward, downward, kept = relay_out(value, extra, order[0])
        arrived = shift(upward, order[0], 1), shift(downward, order[0], SIDE - 1)
        upward, downward = relay_on(kept, arrived)
        later = shift(upward, order[0], 1), shift(downward, order[0], SIDE - 1)
        arrived, _ = lax.optimization_barrier((arrived, (upward, downward)))
        begun.append((kept, arrived, later))

    lower = lax.optimization_barrier(lax.optimization_barrier(tp) == 0)
    south = lax.optimization_barrier(lax.optimization_barrier(tp) < 1)
    upper = lax.optimization_barrier(lax.optimization_barrier(tp) == 1)

    middle = []
    for (kept, arrived, later), (_, order) in zip(begun, GROUPS):
        total, tails = relay_sum(kept, arrived, later)
        lengths = [SIDE, SIDE, SIDE, share, total.shape[-1]]
        lengths[DIMS[order[0]]] = 1
        extra = None
        if tails is not None:
            extra = tap_rows(tails, tap_count, columns, total.shape[-1])
        sent, kept = parts_for(total.reshape(lengths), extra, order[1])
        middle.append((kept, exchange(sent, order[1])))

    values = []
    for kept, arrived in middle:
        value, tails = add_up(kept, arrived)
        values.append(value.reshape(SIDE, 1, 1, share, value.shape[-1]))
        if tails is not None:
            extra = tap_rows(tails, tap_count, columns, 2 * columns)
    both = jnp.concatenate(values, axis=-1)
    sent, kept = parts_for(both, extra, "y")
    arrived = exchange(sent, "y")
    value, tails = add_up(kept, arrived)
    value = value.reshape(share, 2 * columns)
    taps = tap_rows(tails, 8, columns, 2 * columns, factor)

    low, plan, pieces, parts = 0, [], [], []
    for blocks, order in GATHERS:
        part = value[:, 2 * LANES * low : 2 * LANES * (low + blocks)]
        parts.append(gather_over(part, order[0]))
        plan.append((low, order[1], (0,) + HOPS))
        low += blocks
    for part, (_, order) in zip(parts, GATHERS):
        pieces += [part] + exchange([part] * 3, order[1])
    places = jnp.stack([place("z"), place("x")]).astype(jnp.int32)
    grads = finish(places, tuple(plan), pieces, columns, factor)
    grads = [g.reshape(reps * share, columns) for g in grads]

    other_taps = lax.ppermute(taps, "tp", swap)
    grad_taps = [
        jnp.concatenate([jnp.where(left, t, o), jnp.where(right, o, t)], axis=1)
        for left, right, t, o in (
            (lower, south, taps[:3], other_taps[:3]),
            (jnp.logical_not(upper), jnp.logical_not(upper), taps[3:6], other_taps[3:6]),
        )
    ]

    def project(w):
        result = jnp.einsum("nk,dk->nd", stacked, w, preferred_element_type=jnp.float32)
        return result.astype(jnp.bfloat16)

    partials = [project(shard), project(below), project(above)]
    partials.append(jnp.concatenate([project(w) for w in opposite], axis=1))
    away = [lax.dynamic_slice_in_dim(p, (1 - tp) * half, half, 0) for p in partials]
    kept = [lax.dynamic_slice_in_dim(p, tp * half, half, 0) for p in partials]
    got = [lax.ppermute(p, "tp", swap) for p in away]
    grad_inputs = join(jnp.full((1,), place("y"), jnp.int32), kept, got)[None]
    return (grad_inputs, grads[0], grads[1], grad_taps[0], grad_taps[1])


def solution(mesh):
    placed = (
        P(("rep", "fs"), "tp", None),
        P(("rep", "fs"), None, "tp"),
        P(("rep", "fs"), None, "tp"),
        P(("rep", "fs"), None, "tp"),
        P("fs", "tp"),
        P("fs", "tp"),
        P(),
        P(),
    )
    return jax.shard_map(
        layer,
        mesh=mesh,
        in_specs=placed,
        out_specs=(P(("rep", "fs"), "tp", None), P("fs", "tp"), P("fs", "tp"), P(), P()),
        check_vma=False,
    )
```

```python
import functools

import jax
import jax.numpy as jnp
from jax import lax
from jax.experimental import pallas as pl
from jax.experimental.pallas import tpu as pltpu
from jax.sharding import PartitionSpec as P


SIDE = 4
HOPS = (1, 3, 2)
LANES = 128
CHUNK = 32
HALO = 8
GROUPS = ((6, "zx"), (5, "xz"))
GATHERS = ((6, "zx"), (5, "xz"))
DIMS = {"y": 0, "z": 1, "x": 2}


def shift(value, axis, hop):
    ring = range(SIDE)
    if axis == "y":
        return lax.ppermute(value, "fs", [(i, (i + hop) % SIDE) for i in ring])
    if axis == "z":
        pairs = [(z * SIDE + x, (z + hop) % SIDE * SIDE + x) for z in ring for x in ring]
    else:
        pairs = [(z * SIDE + x, z * SIDE + (x + hop) % SIDE) for z in ring for x in ring]
    return lax.ppermute(value, "rep", pairs)


def place(axis):
    if axis == "y":
        return lax.axis_index("fs")
    rep = lax.axis_index("rep")
    return rep // SIDE if axis == "z" else rep % SIDE


def parts_for(value, extra, axis):
    me, dim, width = place(axis), DIMS[axis], value.shape[-1]
    sent = []
    for hop in HOPS:
        part = lax.dynamic_slice_in_dim(value, (me + hop) % SIDE, 1, dim).reshape(-1, width)
        sent.append(part if extra is None else jnp.concatenate([part, extra], axis=0))
    return sent, (lax.dynamic_slice_in_dim(value, me, 1, dim), extra)


def exchange(sent, axis):
    return [shift(part, axis, hop) for hop, part in zip(HOPS, sent)]


def four(own, one, three, two):
    return (own + two) + (one + three)


def tap_kernel(columns, width, scale, *refs):
    out_ref, values = refs[-1], []
    for ref in refs[:-1]:
        rows = ref[...].astype(jnp.float32)
        if rows.shape[0] > 8:
            cut = rows.shape[0] // 2
            both = rows[:cut] + rows[cut:]
            pieces = [both[k : k + 8] for k in range(0, cut, 8)]
            values.append(jnp.concatenate(pieces, axis=1)[:, :columns])
        elif rows.shape[1] == 2 * columns:
            values.append(rows[:, :columns] + rows[:, columns:])
        else:
            values.append(rows)
    total = four(*values) if len(values) == SIDE else jnp.concatenate(values, axis=1)
    if scale is not None:
        out_ref[...] = total * scale
        return
    high = total.astype(jnp.bfloat16).astype(jnp.float32)
    parts = [high, total - high]
    if width == 2 * columns:
        out_ref[...] = jnp.concatenate(parts, axis=1).astype(jnp.bfloat16)
        return
    count = out_ref.shape[0] // 16
    if count * width > columns:
        blank = jnp.zeros((8, count * width - columns), jnp.float32)
        parts = [jnp.concatenate([part, blank], axis=1) for part in parts]
    cuts = [part[:, k * width : (k + 1) * width] for part in parts for k in range(count)]
    out_ref[...] = jnp.concatenate(cuts, axis=0).astype(jnp.bfloat16)


def tap_rows(tails, rows, columns, width, scale=None):
    count = 8 if width == 2 * columns else 16 * (-(-columns // width))
    out = (8, columns) if scale is not None else (count, width)
    kind = jnp.float32 if scale is not None else jnp.bfloat16

    def spec(tail):
        last = tail.shape[0] // rows - 1
        return pl.BlockSpec((rows, tail.shape[1]), lambda j: (last, 0))

    return pl.pallas_call(
        functools.partial(tap_kernel, columns, width, scale),
        grid=(1,),
        in_specs=[spec(tail) for tail in tails],
        out_specs=pl.BlockSpec(out, lambda j: (0, 0)),
        out_shape=jax.ShapeDtypeStruct(out, kind),
        cost_estimate=pl.CostEstimate(flops=100000, bytes_accessed=500000, transcendentals=0),
        compiler_params=pltpu.CompilerParams(vmem_limit_bytes=4 * 1024 * 1024),
        name="tap_rows",
    )(*tails)


def add_up(kept, arrived):
    own, extra = kept
    width, count = own.shape[-1], own.size // own.shape[-1]
    heads = [own.reshape(count, width)] + [part[:count] for part in arrived]
    total = four(*[head.astype(jnp.float32) for head in heads])
    tails = None
    if extra is not None:
        tails = [extra] + arrived
    return total.astype(jnp.bfloat16).reshape(own.shape), tails


def relay_out(value, extra, axis):
    me, dim, width = place(axis), DIMS[axis], value.shape[-1]
    own, right, opposite, left = [
        lax.dynamic_slice_in_dim(value, (me + hop) % SIDE, 1, dim).reshape(-1, width)
        for hop in range(SIDE)
    ]
    cut = own.shape[0] // 2
    tail = [] if extra is None else [extra]
    upward = jnp.concatenate([opposite[:cut], right[cut:]] + tail, axis=0)
    downward = jnp.concatenate([opposite[cut:], left[:cut]] + tail, axis=0)
    return upward, downward, (own, right[:cut], left[cut:], extra)


def relay_on(kept, arrived):
    _, right, left, extra = kept
    cut = right.shape[0]
    below, above = arrived
    upward = (right.astype(jnp.float32) + below[:cut].astype(jnp.float32)).astype(jnp.bfloat16)
    downward = (left.astype(jnp.float32) + above[:cut].astype(jnp.float32)).astype(jnp.bfloat16)
    if extra is not None:
        upward = jnp.concatenate([upward, below[2 * cut :]], axis=0)
    return upward, downward


def relay_sum(kept, arrived, later):
    own, right, _, extra = kept
    cut = right.shape[0]
    below, above = arrived
    top = own[:cut].astype(jnp.float32) + above[cut : 2 * cut].astype(jnp.float32)
    bottom = own[cut:].astype(jnp.float32) + below[cut : 2 * cut].astype(jnp.float32)
    top = top + later[0][:cut].astype(jnp.float32)
    bottom = bottom + later[1].astype(jnp.float32)
    total = jnp.concatenate([top.astype(jnp.bfloat16), bottom.astype(jnp.bfloat16)], axis=0)
    tails = None
    if extra is not None:
        tails = [extra, below, above, later[0]]
    return total, tails


def gather_over(value, axis):
    one, three, two = exchange([value] * 3, axis)
    turn = (place(axis) + SIDE - jnp.arange(SIDE)) % SIDE
    turn = turn.reshape((SIDE,) + (1,) * value.ndim)
    return jnp.where(
        turn == 0, value, jnp.where(turn == 1, one, jnp.where(turn == 2, two, three))
    )


def backward_kernel(tp_ref, gate_ref, up_ref, cot_ref, tap_gate_ref, tap_up_ref, *rest):
    group_ref, stacked_ref, sums_ref, gate_pad, up_pad = rest[-5:]
    length = gate_ref.shape[0]
    zeros = jnp.zeros((HALO, LANES), jnp.float32)
    gate_pad[0:HALO, :] = zeros
    up_pad[0:HALO, :] = zeros
    gate_pad[HALO : HALO + length, :] = gate_ref[...].astype(jnp.float32)
    up_pad[HALO : HALO + length, :] = up_ref[...].astype(jnp.float32)
    kg = tap_gate_ref[...].astype(jnp.float32)
    ku = tap_up_ref[...].astype(jnp.float32)
    kg = [jnp.broadcast_to(kg[j : j + 1], (CHUNK, LANES)) for j in range(3)]
    ku = [jnp.broadcast_to(ku[j : j + 1], (CHUNK, LANES)) for j in range(3)]
    root = 0.7978845608028654
    count = length // CHUNK

    def delayed(pad, row):
        rows = pad[pl.ds(row, CHUNK + HALO), :]
        return [pltpu.roll(rows, 2, 0)[HALO:], pltpu.roll(rows, 1, 0)[HALO:], rows[HALO:]]

    def advanced(now, later, kernel):
        rows = jnp.concatenate([now, later], axis=0)
        one = pltpu.roll(rows, CHUNK + HALO - 1, 0)[:CHUNK]
        two = pltpu.roll(rows, CHUNK + HALO - 2, 0)[:CHUNK]
        return kernel[2] * now + kernel[1] * one + kernel[0] * two

    def folded(product):
        return jnp.sum(product.reshape(CHUNK // 8, 8, LANES), axis=0)

    def step(index, carry):
        later_gate, later_up, sums = carry
        row = pl.multiple_of((count - 1 - index) * CHUNK, CHUNK)
        gates = delayed(gate_pad, row)
        ups = delayed(up_pad, row)
        cot = cot_ref[pl.ds(row, CHUNK), :].astype(jnp.float32)
        v = kg[0] * gates[0] + kg[1] * gates[1] + kg[2] * gates[2]
        mixed_up = ku[0] * ups[0] + ku[1] * ups[1] + ku[2] * ups[2]
        square = v * v
        bent = jnp.tanh(v * (root + (root * 0.044715) * square))
        rise = 0.5 + 0.5 * bent
        slope = rise + (0.5 * v) * (1.0 - bent * bent) * (root + (3.0 * root * 0.044715) * square)
        back_gate = cot * mixed_up * slope
        back_up = cot * (v * rise)
        out_gate = advanced(back_gate, later_gate, kg).astype(jnp.bfloat16)
        out_up = advanced(back_up, later_up, ku).astype(jnp.bfloat16)
        for ref in (group_ref, stacked_ref):
            ref[pl.ds(row, CHUNK), 0:LANES] = out_gate
            ref[pl.ds(row, CHUNK), LANES : 2 * LANES] = out_up
        products = [back_gate * g for g in gates] + [back_up * u for u in ups]
        sums = tuple(s + folded(p) for s, p in zip(sums, products))
        return back_gate[:HALO], back_up[:HALO], sums

    start = (zeros, zeros, (zeros,) * 6)
    sums = lax.fori_loop(0, count, step, start)[2]
    rows = [jnp.sum(s, axis=0, keepdims=True) for s in sums]
    sums_ref[...] = jnp.concatenate(rows + [jnp.zeros((2, LANES), jnp.float32)], axis=0)


def backward(tp, pre_gate, pre_up, cotangent, taps_gate, taps_up, first, blocks, stacked):
    length, columns = pre_gate.shape
    total = columns // LANES
    wide = pl.BlockSpec((length, LANES), lambda j, t: (0, first + j))
    taps = pl.BlockSpec((3, LANES), lambda j, t: (0, t[0] * total + first + j))
    operands = [tp, pre_gate, pre_up, cotangent, taps_gate, taps_up]
    in_specs = [wide, wide, wide, taps, taps]
    aliases = {}
    if stacked is not None:
        aliases = {len(operands): 1}
        operands.append(stacked)
        in_specs.append(pl.BlockSpec(memory_space=pl.ANY))
    return pl.pallas_call(
        backward_kernel,
        grid_spec=pltpu.PrefetchScalarGridSpec(
            num_scalar_prefetch=1,
            grid=(blocks,),
            in_specs=in_specs,
            out_specs=[
                pl.BlockSpec((length, 2 * LANES), lambda j, t: (0, j)),
                pl.BlockSpec((length, 2 * LANES), lambda j, t: (0, first + j)),
                pl.BlockSpec((8, LANES), lambda j, t: (0, j)),
            ],
            scratch_shapes=[pltpu.VMEM((length + HALO, LANES), jnp.float32)] * 2,
        ),
        out_shape=[
            jax.ShapeDtypeStruct((length, blocks * 2 * LANES), jnp.bfloat16),
            jax.ShapeDtypeStruct((length, 2 * columns), jnp.bfloat16),
            jax.ShapeDtypeStruct((8, blocks * LANES), jnp.float32),
        ],
        input_output_aliases=aliases,
        cost_estimate=pl.CostEstimate(
            flops=2000 * length * LANES * blocks,
            bytes_accessed=length * LANES * blocks * 14,
            transcendentals=length * LANES * blocks,
        ),
        compiler_params=pltpu.CompilerParams(vmem_limit_bytes=16 * 1024 * 1024),
        name="backward",
    )(*operands)


def weave_kernel(gate_ref, up_ref, out_ref):
    for block in range(gate_ref.shape[1] // LANES):
        columns = slice(block * LANES, (block + 1) * LANES)
        out_ref[:, 2 * block * LANES : (2 * block + 1) * LANES] = gate_ref[:, columns]
        out_ref[:, (2 * block + 1) * LANES : (2 * block + 2) * LANES] = up_ref[:, columns]


def weave(gate, up):
    rows, columns = gate.shape
    narrow = pl.BlockSpec((rows // SIDE, columns), lambda j: (j, 0))
    return pl.pallas_call(
        weave_kernel,
        grid=(SIDE,),
        in_specs=[narrow, narrow],
        out_specs=pl.BlockSpec((rows // SIDE, 2 * columns), lambda j: (j, 0)),
        out_shape=jax.ShapeDtypeStruct((rows, 2 * columns), gate.dtype),
        cost_estimate=pl.CostEstimate(
            flops=100 * rows * columns, bytes_accessed=8 * rows * columns, transcendentals=0
        ),
        compiler_params=pltpu.CompilerParams(vmem_limit_bytes=8 * 1024 * 1024),
        name="weave",
    )(gate, up)


def join_kernel(place_ref, *refs):
    kept, got, out_ref, sums, sems = refs[:4], refs[4:8], refs[8], refs[9], refs[10]
    width = sums.shape[-1]
    copies = []
    for number, hop in enumerate((0,) + HOPS):
        total = kept[number][...].astype(jnp.float32) + got[number][...].astype(jnp.float32)
        sums[number] = total.astype(jnp.bfloat16)
        source = lax.rem(place_ref[0] + SIDE - hop, SIDE)
        target = out_ref.at[:, pl.ds(pl.multiple_of(source * width, width), width)]
        copies.append(pltpu.make_async_copy(sums.at[number], target, sems.at[number]))
        if number:
            copies[number - 1].start()
    copies[-1].start()
    for copy in copies:
        copy.wait()


def join(place_y, kept, got):
    rows, width = kept[0].shape
    return pl.pallas_call(
        join_kernel,
        in_specs=[pl.BlockSpec(memory_space=pltpu.SMEM)]
        + [pl.BlockSpec(memory_space=pltpu.VMEM)] * (2 * SIDE),
        out_specs=pl.BlockSpec(memory_space=pl.ANY),
        out_shape=jax.ShapeDtypeStruct((rows, SIDE * width), jnp.bfloat16),
        scratch_shapes=[
            pltpu.VMEM((SIDE, rows, width), jnp.bfloat16),
            pltpu.SemaphoreType.DMA((SIDE,)),
        ],
        cost_estimate=pl.CostEstimate(
            flops=400 * rows * width, bytes_accessed=24 * rows * width, transcendentals=0
        ),
        compiler_params=pltpu.CompilerParams(vmem_limit_bytes=10 * 1024 * 1024),
        name="join",
    )(place_y, *kept, *got)


def finish_kernel(plan, factor, places, *refs):
    count = sum(len(lists) for _, _, lists in plan)
    pieces, outs = refs[:count], refs[count : count + 2]
    halves, sems = refs[count + 2 : -1], refs[-1]
    copies, number = [], 0

    def begin(index):
        for copy in copies[2 * index : 2 * index + 2]:
            copy.start()

    for low, axis, hops in plan:
        me = places[0] if axis == "z" else places[1]
        for hop in hops:
            piece, half = pieces[number], halves[number]
            width = piece.shape[-1] // 2
            for block in range(width // LANES):
                values = piece[:, :, 2 * block * LANES : 2 * (block + 1) * LANES]
                values = values.astype(jnp.float32) * factor
                half[0, :, :, block * LANES : (block + 1) * LANES] = values[:, :, :LANES]
                half[1, :, :, block * LANES : (block + 1) * LANES] = values[:, :, LANES:]
            source = lax.rem(me + SIDE - hop, SIDE)
            for side in range(2):
                columns = pl.ds(low * LANES, width)
                if axis == "z":
                    target = outs[side].at[source, :, :, columns]
                else:
                    target = outs[side].at[:, source, :, columns]
                copies.append(pltpu.make_async_copy(half.at[side], target, sems.at[number, side]))
            if number:
                begin(number - 1)
            number += 1
    begin(number - 1)
    for copy in copies:
        copy.wait()


def finish(places, plan, pieces, columns, factor):
    share = pieces[0].shape[1]
    out = jax.ShapeDtypeStruct((SIDE, SIDE, share, columns), jnp.float32)
    size = SIDE * SIDE * share * columns
    return pl.pallas_call(
        functools.partial(finish_kernel, plan, factor),
        in_specs=[pl.BlockSpec(memory_space=pltpu.SMEM)]
        + [pl.BlockSpec(memory_space=pltpu.VMEM)] * len(pieces),
        out_specs=[pl.BlockSpec(memory_space=pl.ANY)] * 2,
        out_shape=[out, out],
        scratch_shapes=[
            pltpu.VMEM((2, SIDE, share, p.shape[-1] // 2), jnp.float32) for p in pieces
        ]
        + [pltpu.SemaphoreType.DMA((len(pieces), 2))],
        cost_estimate=pl.CostEstimate(
            flops=200 * size, bytes_accessed=12 * size, transcendentals=0
        ),
        compiler_params=pltpu.CompilerParams(vmem_limit_bytes=16 * 1024 * 1024),
        name="finish",
    )(places, *pieces)


def layer(inputs, pre_gate, pre_up, cotangent, w_gate, w_up, taps_gate, taps_up):
    columns = pre_gate.shape[2]
    reps, shards = lax.axis_size("rep"), lax.axis_size("fs")
    share = w_gate.shape[0] // reps
    tp = lax.axis_index("tp")
    swap = [(0, 1), (1, 0)]
    factor = float(pre_gate.shape[1] * reps * shards) ** (-0.5)

    shard = weave(w_gate, w_up)
    below, above = shift(shard, "y", 1), shift(shard, "y", SIDE - 1)
    middle_row = shard.shape[0] // 2
    opposite = [shift(below[:middle_row], "y", 1), shift(above[middle_row:], "y", SIDE - 1)]

    half = inputs.shape[1]
    own_rows = inputs[0]
    other_rows = lax.ppermute(own_rows, "tp", swap)
    first = jnp.where(tp == 0, own_rows, other_rows)
    second = jnp.where(tp == 0, other_rows, own_rows)
    whole_rows = jnp.concatenate([first, second], axis=0)

    where = jnp.full((1,), tp, jnp.int32)
    stacked, low, tap_sums, begun, extra = None, 0, [], [], None
    for number, (blocks, order) in enumerate(GROUPS):
        group, stacked, taps = backward(
            where, pre_gate[0], pre_up[0], cotangent[0], taps_gate, taps_up, low, blocks, stacked
        )
        low += blocks
        tap_sums.append(taps)
        width = group.shape[1]
        if number == len(GROUPS) - 1:
            extra = tap_rows(tap_sums, 8, columns, width)
            tap_count = extra.shape[0]
        value = jnp.einsum("nd,nk->dk", whole_rows, group, preferred_element_type=jnp.float32)
        value = value.astype(jnp.bfloat16).reshape(SIDE, SIDE, SIDE, share, width)
        upward, downward, kept = relay_out(value, extra, order[0])
        arrived = shift(upward, order[0], 1), shift(downward, order[0], SIDE - 1)
        upward, downward = relay_on(kept, arrived)
        later = shift(upward, order[0], 1), shift(downward, order[0], SIDE - 1)
        arrived, _ = lax.optimization_barrier((arrived, (upward, downward)))
        begun.append((kept, arrived, later))

    lower = lax.optimization_barrier(lax.optimization_barrier(tp) == 0)
    south = lax.optimization_barrier(lax.optimization_barrier(tp) < 1)
    north = lax.optimization_barrier(lax.optimization_barrier(tp) > 0)
    upper = lax.optimization_barrier(lax.optimization_barrier(tp) == 1)

    middle = []
    for (kept, arrived, later), (_, order) in zip(begun, GROUPS):
        total, tails = relay_sum(kept, arrived, later)
        lengths = [SIDE, SIDE, SIDE, share, total.shape[-1]]
        lengths[DIMS[order[0]]] = 1
        extra = None
        if tails is not None:
            extra = tap_rows(tails, tap_count, columns, total.shape[-1])
        sent, kept = parts_for(total.reshape(lengths), extra, order[1])
        middle.append((kept, exchange(sent, order[1])))

    values = []
    for kept, arrived in middle:
        value, tails = add_up(kept, arrived)
        values.append(value.reshape(SIDE, 1, 1, share, value.shape[-1]))
        if tails is not None:
            extra = tap_rows(tails, tap_count, columns, 2 * columns)
    both = jnp.concatenate(values, axis=-1)
    sent, kept = parts_for(both, extra, "y")
    arrived = exchange(sent, "y")
    value, tails = add_up(kept, arrived)
    value = value.reshape(share, 2 * columns)
    taps = tap_rows(tails, 8, columns, 2 * columns, factor)

    low, plan, pieces, parts = 0, [], [], []
    for blocks, order in GATHERS:
        part = value[:, 2 * LANES * low : 2 * LANES * (low + blocks)]
        parts.append(gather_over(part, order[0]))
        plan.append((low, order[1], (0,) + HOPS))
        low += blocks
    for part, (_, order) in zip(parts, GATHERS):
        pieces += [part] + exchange([part] * 3, order[1])
    places = jnp.stack([place("z"), place("x")]).astype(jnp.int32)
    grads = finish(places, tuple(plan), pieces, columns, factor)
    grads = [g.reshape(reps * share, columns) for g in grads]

    other_taps = lax.ppermute(taps, "tp", swap)
    grad_taps = [
        jnp.concatenate([jnp.where(left, t, o), jnp.where(right, o, t)], axis=1)
        for left, right, t, o in (
            (lower, south, taps[:3], other_taps[:3]),
            (jnp.logical_not(upper), jnp.logical_not(north), taps[3:6], other_taps[3:6]),
        )
    ]

    def project(w):
        result = jnp.einsum("nk,dk->nd", stacked, w, preferred_element_type=jnp.float32)
        return result.astype(jnp.bfloat16)

    partials = [project(shard), project(below), project(above)]
    partials.append(jnp.concatenate([project(w) for w in opposite], axis=1))
    away = [lax.dynamic_slice_in_dim(p, (1 - tp) * half, half, 0) for p in partials]
    kept = [lax.dynamic_slice_in_dim(p, tp * half, half, 0) for p in partials]
    got = [lax.ppermute(p, "tp", swap) for p in away]
    grad_inputs = join(jnp.full((1,), place("y"), jnp.int32), kept, got)[None]
    return (grad_inputs, grads[0], grads[1], grad_taps[0], grad_taps[1])


def solution(mesh):
    placed = (
        P(("rep", "fs"), "tp", None),
        P(("rep", "fs"), None, "tp"),
        P(("rep", "fs"), None, "tp"),
        P(("rep", "fs"), None, "tp"),
        P("fs", "tp"),
        P("fs", "tp"),
        P(),
        P(),
    )
    return jax.shard_map(
        layer,
        mesh=mesh,
        in_specs=placed,
        out_specs=(P(("rep", "fs"), "tp", None), P("fs", "tp"), P("fs", "tp"), P(), P()),
        check_vma=False,
    )
```

```python
import functools

import jax
import jax.numpy as jnp
from jax import lax
from jax.experimental import pallas as pl
from jax.experimental.pallas import tpu as pltpu
from jax.sharding import PartitionSpec as P


SIDE = 4
HOPS = (1, 3, 2)
LANES = 128
CHUNK = 32
HALO = 8
GROUPS = ((6, "zx"), (5, "xz"))
GATHERS = ((6, "zx"), (5, "xz"))
DIMS = {"y": 0, "z": 1, "x": 2}


def shift(value, axis, hop):
    ring = range(SIDE)
    if axis == "y":
        return lax.ppermute(value, "fs", [(i, (i + hop) % SIDE) for i in ring])
    if axis == "z":
        pairs = [(z * SIDE + x, (z + hop) % SIDE * SIDE + x) for z in ring for x in ring]
    else:
        pairs = [(z * SIDE + x, z * SIDE + (x + hop) % SIDE) for z in ring for x in ring]
    return lax.ppermute(value, "rep", pairs)


def place(axis):
    if axis == "y":
        return lax.axis_index("fs")
    rep = lax.axis_index("rep")
    return rep // SIDE if axis == "z" else rep % SIDE


def parts_for(value, extra, axis):
    me, dim, width = place(axis), DIMS[axis], value.shape[-1]
    sent = []
    for hop in HOPS:
        part = lax.dynamic_slice_in_dim(value, (me + hop) % SIDE, 1, dim).reshape(-1, width)
        sent.append(part if extra is None else jnp.concatenate([part, extra], axis=0))
    return sent, (lax.dynamic_slice_in_dim(value, me, 1, dim), extra)


def exchange(sent, axis):
    return [shift(part, axis, hop) for hop, part in zip(HOPS, sent)]


def four(own, one, three, two):
    return (own + two) + (one + three)


def tap_kernel(columns, width, scale, *refs):
    out_ref, values = refs[-1], []
    for ref in refs[:-1]:
        rows = ref[...].astype(jnp.float32)
        if rows.shape[0] > 8:
            cut = rows.shape[0] // 2
            both = rows[:cut] + rows[cut:]
            pieces = [both[k : k + 8] for k in range(0, cut, 8)]
            values.append(jnp.concatenate(pieces, axis=1)[:, :columns])
        elif rows.shape[1] == 2 * columns:
            values.append(rows[:, :columns] + rows[:, columns:])
        else:
            values.append(rows)
    total = four(*values) if len(values) == SIDE else jnp.concatenate(values, axis=1)
    if scale is not None:
        out_ref[...] = total * scale
        return
    high = total.astype(jnp.bfloat16).astype(jnp.float32)
    parts = [high, total - high]
    if width == 2 * columns:
        out_ref[...] = jnp.concatenate(parts, axis=1).astype(jnp.bfloat16)
        return
    count = out_ref.shape[0] // 16
    if count * width > columns:
        blank = jnp.zeros((8, count * width - columns), jnp.float32)
        parts = [jnp.concatenate([part, blank], axis=1) for part in parts]
    cuts = [part[:, k * width : (k + 1) * width] for part in parts for k in range(count)]
    out_ref[...] = jnp.concatenate(cuts, axis=0).astype(jnp.bfloat16)


def tap_rows(tails, rows, columns, width, scale=None):
    count = 8 if width == 2 * columns else 16 * (-(-columns // width))
    out = (8, columns) if scale is not None else (count, width)
    kind = jnp.float32 if scale is not None else jnp.bfloat16

    def spec(tail):
        last = tail.shape[0] // rows - 1
        return pl.BlockSpec((rows, tail.shape[1]), lambda j: (last, 0))

    return pl.pallas_call(
        functools.partial(tap_kernel, columns, width, scale),
        grid=(1,),
        in_specs=[spec(tail) for tail in tails],
        out_specs=pl.BlockSpec(out, lambda j: (0, 0)),
        out_shape=jax.ShapeDtypeStruct(out, kind),
        cost_estimate=pl.CostEstimate(flops=100000, bytes_accessed=500000, transcendentals=0),
        compiler_params=pltpu.CompilerParams(vmem_limit_bytes=4 * 1024 * 1024),
        name="tap_rows",
    )(*tails)


def add_up(kept, arrived):
    own, extra = kept
    width, count = own.shape[-1], own.size // own.shape[-1]
    heads = [own.reshape(count, width)] + [part[:count] for part in arrived]
    total = four(*[head.astype(jnp.float32) for head in heads])
    tails = None
    if extra is not None:
        tails = [extra] + arrived
    return total.astype(jnp.bfloat16).reshape(own.shape), tails


def relay_out(value, extra, axis):
    me, dim, width = place(axis), DIMS[axis], value.shape[-1]
    own, right, opposite, left = [
        lax.dynamic_slice_in_dim(value, (me + hop) % SIDE, 1, dim).reshape(-1, width)
        for hop in range(SIDE)
    ]
    cut = own.shape[0] // 2
    tail = [] if extra is None else [extra]
    upward = jnp.concatenate([opposite[:cut], right[cut:]] + tail, axis=0)
    downward = jnp.concatenate([opposite[cut:], left[:cut]] + tail, axis=0)
    return upward, downward, (own, right[:cut], left[cut:], extra)


def relay_on(kept, arrived):
    _, right, left, extra = kept
    cut = right.shape[0]
    below, above = arrived
    upward = (right.astype(jnp.float32) + below[:cut].astype(jnp.float32)).astype(jnp.bfloat16)
    downward = (left.astype(jnp.float32) + above[:cut].astype(jnp.float32)).astype(jnp.bfloat16)
    if extra is not None:
        upward = jnp.concatenate([upward, below[2 * cut :]], axis=0)
    return upward, downward


def relay_sum(kept, arrived, later):
    own, right, _, extra = kept
    cut = right.shape[0]
    below, above = arrived
    top = own[:cut].astype(jnp.float32) + above[cut : 2 * cut].astype(jnp.float32)
    bottom = own[cut:].astype(jnp.float32) + below[cut : 2 * cut].astype(jnp.float32)
    top = top + later[0][:cut].astype(jnp.float32)
    bottom = bottom + later[1].astype(jnp.float32)
    total = jnp.concatenate([top.astype(jnp.bfloat16), bottom.astype(jnp.bfloat16)], axis=0)
    tails = None
    if extra is not None:
        tails = [extra, below, above, later[0]]
    return total, tails


def gather_over(value, axis):
    one, three, two = exchange([value] * 3, axis)
    turn = (place(axis) + SIDE - jnp.arange(SIDE)) % SIDE
    turn = turn.reshape((SIDE,) + (1,) * value.ndim)
    return jnp.where(
        turn == 0, value, jnp.where(turn == 1, one, jnp.where(turn == 2, two, three))
    )


def backward_kernel(tp_ref, gate_ref, up_ref, cot_ref, tap_gate_ref, tap_up_ref, *rest):
    group_ref, stacked_ref, sums_ref, gate_pad, up_pad = rest[-5:]
    length = gate_ref.shape[0]
    zeros = jnp.zeros((HALO, LANES), jnp.float32)
    gate_pad[0:HALO, :] = zeros
    up_pad[0:HALO, :] = zeros
    gate_pad[HALO : HALO + length, :] = gate_ref[...].astype(jnp.float32)
    up_pad[HALO : HALO + length, :] = up_ref[...].astype(jnp.float32)
    kg = tap_gate_ref[...].astype(jnp.float32)
    ku = tap_up_ref[...].astype(jnp.float32)
    kg = [jnp.broadcast_to(kg[j : j + 1], (CHUNK, LANES)) for j in range(3)]
    ku = [jnp.broadcast_to(ku[j : j + 1], (CHUNK, LANES)) for j in range(3)]
    root = 0.7978845608028654
    count = length // CHUNK

    def delayed(pad, row):
        rows = pad[pl.ds(row, CHUNK + HALO), :]
        return [pltpu.roll(rows, 2, 0)[HALO:], pltpu.roll(rows, 1, 0)[HALO:], rows[HALO:]]

    def advanced(now, later, kernel):
        rows = jnp.concatenate([now, later], axis=0)
        one = pltpu.roll(rows, CHUNK + HALO - 1, 0)[:CHUNK]
        two = pltpu.roll(rows, CHUNK + HALO - 2, 0)[:CHUNK]
        return kernel[2] * now + kernel[1] * one + kernel[0] * two

    def folded(product):
        return jnp.sum(product.reshape(CHUNK // 8, 8, LANES), axis=0)

    def step(index, carry):
        later_gate, later_up, sums = carry
        row = pl.multiple_of((count - 1 - index) * CHUNK, CHUNK)
        gates = delayed(gate_pad, row)
        ups = delayed(up_pad, row)
        cot = cot_ref[pl.ds(row, CHUNK), :].astype(jnp.float32)
        v = kg[0] * gates[0] + kg[1] * gates[1] + kg[2] * gates[2]
        mixed_up = ku[0] * ups[0] + ku[1] * ups[1] + ku[2] * ups[2]
        square = v * v
        bent = jnp.tanh(v * (root + (root * 0.044715) * square))
        rise = 0.5 + 0.5 * bent
        slope = rise + (0.5 * v) * (1.0 - bent * bent) * (root + (3.0 * root * 0.044715) * square)
        back_gate = cot * mixed_up * slope
        back_up = cot * (v * rise)
        out_gate = advanced(back_gate, later_gate, kg).astype(jnp.bfloat16)
        out_up = advanced(back_up, later_up, ku).astype(jnp.bfloat16)
        for ref in (group_ref, stacked_ref):
            ref[pl.ds(row, CHUNK), 0:LANES] = out_gate
            ref[pl.ds(row, CHUNK), LANES : 2 * LANES] = out_up
        products = [back_gate * g for g in gates] + [back_up * u for u in ups]
        sums = tuple(s + folded(p) for s, p in zip(sums, products))
        return back_gate[:HALO], back_up[:HALO], sums

    start = (zeros, zeros, (zeros,) * 6)
    sums = lax.fori_loop(0, count, step, start)[2]
    rows = [jnp.sum(s, axis=0, keepdims=True) for s in sums]
    sums_ref[...] = jnp.concatenate(rows + [jnp.zeros((2, LANES), jnp.float32)], axis=0)


def backward(tp, pre_gate, pre_up, cotangent, taps_gate, taps_up, first, blocks, stacked):
    length, columns = pre_gate.shape
    total = columns // LANES
    wide = pl.BlockSpec((length, LANES), lambda j, t: (0, first + j))
    taps = pl.BlockSpec((3, LANES), lambda j, t: (0, t[0] * total + first + j))
    operands = [tp, pre_gate, pre_up, cotangent, taps_gate, taps_up]
    in_specs = [wide, wide, wide, taps, taps]
    aliases = {}
    if stacked is not None:
        aliases = {len(operands): 1}
        operands.append(stacked)
        in_specs.append(pl.BlockSpec(memory_space=pl.ANY))
    return pl.pallas_call(
        backward_kernel,
        grid_spec=pltpu.PrefetchScalarGridSpec(
            num_scalar_prefetch=1,
            grid=(blocks,),
            in_specs=in_specs,
            out_specs=[
                pl.BlockSpec((length, 2 * LANES), lambda j, t: (0, j)),
                pl.BlockSpec((length, 2 * LANES), lambda j, t: (0, first + j)),
                pl.BlockSpec((8, LANES), lambda j, t: (0, j)),
            ],
            scratch_shapes=[pltpu.VMEM((length + HALO, LANES), jnp.float32)] * 2,
        ),
        out_shape=[
            jax.ShapeDtypeStruct((length, blocks * 2 * LANES), jnp.bfloat16),
            jax.ShapeDtypeStruct((length, 2 * columns), jnp.bfloat16),
            jax.ShapeDtypeStruct((8, blocks * LANES), jnp.float32),
        ],
        input_output_aliases=aliases,
        cost_estimate=pl.CostEstimate(
            flops=2000 * length * LANES * blocks,
            bytes_accessed=length * LANES * blocks * 14,
            transcendentals=length * LANES * blocks,
        ),
        compiler_params=pltpu.CompilerParams(
            vmem_limit_bytes=(16 if first else 58) * 1024 * 1024
        ),
        name="backward",
    )(*operands)


def weave_kernel(gate_ref, up_ref, out_ref):
    for block in range(gate_ref.shape[1] // LANES):
        columns = slice(block * LANES, (block + 1) * LANES)
        out_ref[:, 2 * block * LANES : (2 * block + 1) * LANES] = gate_ref[:, columns]
        out_ref[:, (2 * block + 1) * LANES : (2 * block + 2) * LANES] = up_ref[:, columns]


def weave(gate, up):
    rows, columns = gate.shape
    narrow = pl.BlockSpec((rows // SIDE, columns), lambda j: (j, 0))
    return pl.pallas_call(
        weave_kernel,
        grid=(SIDE,),
        in_specs=[narrow, narrow],
        out_specs=pl.BlockSpec((rows // SIDE, 2 * columns), lambda j: (j, 0)),
        out_shape=jax.ShapeDtypeStruct((rows, 2 * columns), gate.dtype),
        cost_estimate=pl.CostEstimate(
            flops=100 * rows * columns, bytes_accessed=8 * rows * columns, transcendentals=0
        ),
        name="weave",
    )(gate, up)


def join_kernel(place_ref, *refs):
    kept, got, out_ref, sums, sems = refs[:4], refs[4:8], refs[8], refs[9], refs[10]
    width = sums.shape[-1]
    copies = []
    for number, hop in enumerate((0,) + HOPS):
        total = kept[number][...].astype(jnp.float32) + got[number][...].astype(jnp.float32)
        sums[number] = total.astype(jnp.bfloat16)
        source = lax.rem(place_ref[0] + SIDE - hop, SIDE)
        target = out_ref.at[:, pl.ds(pl.multiple_of(source * width, width), width)]
        copies.append(pltpu.make_async_copy(sums.at[number], target, sems.at[number]))
        if number:
            copies[number - 1].start()
    copies[-1].start()
    for copy in copies:
        copy.wait()


def join(place_y, kept, got):
    rows, width = kept[0].shape
    return pl.pallas_call(
        join_kernel,
        in_specs=[pl.BlockSpec(memory_space=pltpu.SMEM)]
        + [pl.BlockSpec(memory_space=pltpu.VMEM)] * (2 * SIDE),
        out_specs=pl.BlockSpec(memory_space=pl.ANY),
        out_shape=jax.ShapeDtypeStruct((rows, SIDE * width), jnp.bfloat16),
        scratch_shapes=[
            pltpu.VMEM((SIDE, rows, width), jnp.bfloat16),
            pltpu.SemaphoreType.DMA((SIDE,)),
        ],
        cost_estimate=pl.CostEstimate(
            flops=400 * rows * width, bytes_accessed=24 * rows * width, transcendentals=0
        ),
        compiler_params=pltpu.CompilerParams(vmem_limit_bytes=10 * 1024 * 1024),
        name="join",
    )(place_y, *kept, *got)


def finish_kernel(plan, factor, places, *refs):
    count = sum(len(lists) for _, _, lists in plan)
    pieces, outs = refs[:count], refs[count : count + 2]
    halves, sems = refs[count + 2 : -1], refs[-1]
    copies, number = [], 0

    def begin(index):
        for copy in copies[2 * index : 2 * index + 2]:
            copy.start()

    for low, axis, hops in plan:
        me = places[0] if axis == "z" else places[1]
        for hop in hops:
            piece, half = pieces[number], halves[number]
            width = piece.shape[-1] // 2
            for block in range(width // LANES):
                values = piece[:, :, 2 * block * LANES : 2 * (block + 1) * LANES]
                values = values.astype(jnp.float32) * factor
                half[0, :, :, block * LANES : (block + 1) * LANES] = values[:, :, :LANES]
                half[1, :, :, block * LANES : (block + 1) * LANES] = values[:, :, LANES:]
            source = lax.rem(me + SIDE - hop, SIDE)
            for side in range(2):
                columns = pl.ds(low * LANES, width)
                if axis == "z":
                    target = outs[side].at[source, :, :, columns]
                else:
                    target = outs[side].at[:, source, :, columns]
                copies.append(pltpu.make_async_copy(half.at[side], target, sems.at[number, side]))
            if number:
                begin(number - 1)
            number += 1
    begin(number - 1)
    for copy in copies:
        copy.wait()


def finish(places, plan, pieces, columns, factor):
    share = pieces[0].shape[1]
    out = jax.ShapeDtypeStruct((SIDE, SIDE, share, columns), jnp.float32)
    size = SIDE * SIDE * share * columns
    return pl.pallas_call(
        functools.partial(finish_kernel, plan, factor),
        in_specs=[pl.BlockSpec(memory_space=pltpu.SMEM)]
        + [pl.BlockSpec(memory_space=pltpu.VMEM)] * len(pieces),
        out_specs=[pl.BlockSpec(memory_space=pl.ANY)] * 2,
        out_shape=[out, out],
        scratch_shapes=[
            pltpu.VMEM((2, SIDE, share, p.shape[-1] // 2), jnp.float32) for p in pieces
        ]
        + [pltpu.SemaphoreType.DMA((len(pieces), 2))],
        cost_estimate=pl.CostEstimate(
            flops=200 * size, bytes_accessed=12 * size, transcendentals=0
        ),
        compiler_params=pltpu.CompilerParams(vmem_limit_bytes=16 * 1024 * 1024),
        name="finish",
    )(places, *pieces)


def layer(inputs, pre_gate, pre_up, cotangent, w_gate, w_up, taps_gate, taps_up):
    columns = pre_gate.shape[2]
    reps, shards = lax.axis_size("rep"), lax.axis_size("fs")
    share = w_gate.shape[0] // reps
    tp = lax.axis_index("tp")
    swap = [(0, 1), (1, 0)]
    factor = float(pre_gate.shape[1] * reps * shards) ** (-0.5)

    shard = weave(w_gate, w_up)
    below, above = shift(shard, "y", 1), shift(shard, "y", SIDE - 1)
    middle_row = shard.shape[0] // 2
    opposite = [shift(below[:middle_row], "y", 1), shift(above[middle_row:], "y", SIDE - 1)]

    half = inputs.shape[1]
    own_rows = inputs[0]
    other_rows = lax.ppermute(own_rows, "tp", swap)
    first = jnp.where(tp == 0, own_rows, other_rows)
    second = jnp.where(tp == 0, other_rows, own_rows)
    whole_rows = jnp.concatenate([first, second], axis=0)

    where = jnp.full((1,), tp, jnp.int32)
    stacked, low, tap_sums, begun, extra = None, 0, [], [], None
    for number, (blocks, order) in enumerate(GROUPS):
        group, stacked, taps = backward(
            where, pre_gate[0], pre_up[0], cotangent[0], taps_gate, taps_up, low, blocks, stacked
        )
        low += blocks
        tap_sums.append(taps)
        width = group.shape[1]
        if number == len(GROUPS) - 1:
            extra = tap_rows(tap_sums, 8, columns, width)
            tap_count = extra.shape[0]
        value = jnp.einsum("nd,nk->dk", whole_rows, group, preferred_element_type=jnp.float32)
        value = value.astype(jnp.bfloat16).reshape(SIDE, SIDE, SIDE, share, width)
        upward, downward, kept = relay_out(value, extra, order[0])
        arrived = shift(upward, order[0], 1), shift(downward, order[0], SIDE - 1)
        upward, downward = relay_on(kept, arrived)
        later = shift(upward, order[0], 1), shift(downward, order[0], SIDE - 1)
        arrived, _ = lax.optimization_barrier((arrived, (upward, downward)))
        begun.append((kept, arrived, later))

    lower = lax.optimization_barrier(lax.optimization_barrier(tp) == 0)
    south = lax.optimization_barrier(lax.optimization_barrier(tp) < 1)
    north = lax.optimization_barrier(lax.optimization_barrier(tp) > 0)
    upper = lax.optimization_barrier(lax.optimization_barrier(tp) == 1)

    middle = []
    for (kept, arrived, later), (_, order) in zip(begun, GROUPS):
        total, tails = relay_sum(kept, arrived, later)
        lengths = [SIDE, SIDE, SIDE, share, total.shape[-1]]
        lengths[DIMS[order[0]]] = 1
        extra = None
        if tails is not None:
            extra = tap_rows(tails, tap_count, columns, total.shape[-1])
        sent, kept = parts_for(total.reshape(lengths), extra, order[1])
        middle.append((kept, exchange(sent, order[1])))

    values = []
    for kept, arrived in middle:
        value, tails = add_up(kept, arrived)
        values.append(value.reshape(SIDE, 1, 1, share, value.shape[-1]))
        if tails is not None:
            extra = tap_rows(tails, tap_count, columns, 2 * columns)
    both = jnp.concatenate(values, axis=-1)
    sent, kept = parts_for(both, extra, "y")
    arrived = exchange(sent, "y")
    value, tails = add_up(kept, arrived)
    value = value.reshape(share, 2 * columns)
    taps = tap_rows(tails, 8, columns, 2 * columns, factor)

    low, plan, pieces, parts = 0, [], [], []
    for blocks, order in GATHERS:
        part = value[:, 2 * LANES * low : 2 * LANES * (low + blocks)]
        parts.append(gather_over(part, order[0]))
        plan.append((low, order[1], (0,) + HOPS))
        low += blocks
    for part, (_, order) in zip(parts, GATHERS):
        pieces += [part] + exchange([part] * 3, order[1])
    places = jnp.stack([place("z"), place("x")]).astype(jnp.int32)
    grads = finish(places, tuple(plan), pieces, columns, factor)
    grads = [g.reshape(reps * share, columns) for g in grads]

    other_taps = lax.ppermute(taps, "tp", swap)
    grad_taps = [
        jnp.concatenate([jnp.where(left, t, o), jnp.where(right, o, t)], axis=1)
        for left, right, t, o in (
            (lower, south, taps[:3], other_taps[:3]),
            (jnp.logical_not(upper), jnp.logical_not(north), taps[3:6], other_taps[3:6]),
        )
    ]

    def project(w):
        result = jnp.einsum("nk,dk->nd", stacked, w, preferred_element_type=jnp.float32)
        return result.astype(jnp.bfloat16)

    partials = [project(shard), project(below), project(above)]
    partials.append(jnp.concatenate([project(w) for w in opposite], axis=1))
    away = [lax.dynamic_slice_in_dim(p, (1 - tp) * half, half, 0) for p in partials]
    kept = [lax.dynamic_slice_in_dim(p, tp * half, half, 0) for p in partials]
    got = [lax.ppermute(p, "tp", swap) for p in away]
    grad_inputs = join(jnp.full((1,), place("y"), jnp.int32), kept, got)[None]
    return (grad_inputs, grads[0], grads[1], grad_taps[0], grad_taps[1])


def solution(mesh):
    placed = (
        P(("rep", "fs"), "tp", None),
        P(("rep", "fs"), None, "tp"),
        P(("rep", "fs"), None, "tp"),
        P(("rep", "fs"), None, "tp"),
        P("fs", "tp"),
        P("fs", "tp"),
        P(),
        P(),
    )
    return jax.shard_map(
        layer,
        mesh=mesh,
        in_specs=placed,
        out_specs=(P(("rep", "fs"), "tp", None), P("fs", "tp"), P("fs", "tp"), P(), P()),
        check_vma=False,
    )
```
